256 devices in a mesh: kv: 16 (over y, x), tp: 16 (over z, core).
Axes of the slice: x: 4, y: 4, z: 8, core: 2. Of those that a mesh axis runs over, the one named last changes fastest.
Arguments:
- tokens: bfloat16 [1536, 4096], P('kv', 'tp'), may hold values from -20 to 20
- state: float32 [1536, 32, 4096], P('kv', 'tp'), may hold values from -4 to 4
- w_query: bfloat16 [4096, 2048], P(None, 'tp'), may hold values from -0.09375 to 0.09375
- w_key: bfloat16 [4096, 2048], P(None, 'tp'), may hold values from -0.09375 to 0.09375
- w_value: bfloat16 [4096, 2048], P(None, 'tp'), may hold values from -0.09375 to 0.09375
- w_gate: bfloat16 [4096, 2048], P(None, 'tp'), may hold values from -0.09375 to 0.09375
- w_decay: bfloat16 [4096, 32], replicated, may hold values from -0.09375 to 0.09375
- w_beta: bfloat16 [4096, 32], replicated, may hold values from -0.09375 to 0.09375
- decay_rate: float32 [32], P('tp'), may hold values from 0.03 to 3
- decay_bias: float32 [32], P('tp'), may hold values from -1 to 1
- mix_gain: float32 [4096], replicated, may hold values from 0.1 to 1.9
- out_gain: float32 [64], replicated, may hold values from 0.1 to 1.9
- w_out: bfloat16 [2048, 4096], P('tp'), may hold values from -0.125 to 0.125
- ffn_gain: float32 [4096], replicated, may hold values from 0.1 to 1.9
- w_up: bfloat16 [4096, 16384], P('tp', 'kv'), may hold values from -0.09375 to 0.09375
- w_down: bfloat16 [16384, 4096], P('kv', 'tp'), may hold values from -0.046875 to 0.046875
Outputs:
- mixed: bfloat16 [1536, 4096], P('kv', 'tp')
- new_state: float32 [1536, 32, 4096], P('kv', 'tp')
The draws below stay inside these ranges and needn't reach their ends.
All inputs are finite; a program needn't handle non-finite values.
Results may differ from the reference program's by a relative error of at most 0.024.
Values may be sent and summed in bfloat16 or wider, within the bound.
No kernel may reach another device: no remote copies, remote signals or barrier semaphores. Data moves between devices by JAX's collectives and lax.ppermute only.
A program may use at most 64 MiB of HBM per device.

```python
import math
import jax
import jax.numpy as jnp
from jax import lax

D = 4096
HEADS = 32
HEAD_DIM = 64
FF = 16384
BATCH = 1536


def draw_tokens(key, part):
    scale_key, base_key = jax.random.split(jax.random.fold_in(key, 11))
    scales = jnp.exp(jax.random.uniform(scale_key, (D // 32,), jnp.float32, -1.2, 1.2))
    column_scales = jnp.repeat(scales, 32)
    base = jnp.clip(jax.random.normal(base_key, (BATCH, D), jnp.float32), -6.0, 6.0)
    return (base * column_scales[None, :]).astype(jnp.bfloat16)


def levels(stream_key, shape, cuts, smallest, top_value):
    def one(axis_at, shards_of):
        heights = jax.random.uniform(jax.random.fold_in(jax.random.fold_in(stream_key, 6), axis_at), (shards_of,), jnp.float32, smallest / len(cuts), top_value / len(cuts))
        return jnp.repeat(jnp.exp(heights), shape[axis_at] // shards_of).reshape((-1,) + (1,) * (len(shape) - axis_at - 1))

    gain = one(*cuts[0])
    for cut in cuts[1:]:
        gain = gain * one(*cut)
    return gain


def gaussian(key, shape, scale, limit, cuts=(), kind=jnp.bfloat16):
    level = levels(key, shape, cuts, -0.22, 0.18) if cuts else 1.0
    result = jax.random.normal(key, shape, jnp.float32) * scale * level
    return jnp.minimum(jnp.maximum(result, -limit), limit).astype(kind)


def setup_inputs(seed: int = 0) -> dict:
    splits = jax.random.split(jax.random.key(seed), 17)
    tokens = draw_tokens(jax.random.fold_in(splits[16], 71), 0)
    state = gaussian(splits[1], (BATCH, HEADS, HEAD_DIM * HEAD_DIM), 0.5, 4.0, ((0, 16), (1, 16)), jnp.float32)
    w_query = gaussian(splits[2], (D, HEADS * HEAD_DIM), D ** -0.5, 0.09375, ((1, 16),))
    w_key = gaussian(splits[3], (D, HEADS * HEAD_DIM), D ** -0.5, 0.09375, ((1, 16),))
    w_value = gaussian(splits[4], (D, HEADS * HEAD_DIM), D ** -0.5, 0.09375, ((1, 16),))
    w_gate = gaussian(splits[5], (D, HEADS * HEAD_DIM), D ** -0.5, 0.09375, ((1, 16),))
    w_decay = gaussian(splits[6], (D, HEADS), D ** -0.5, 0.09375)
    w_beta = gaussian(splits[7], (D, HEADS), D ** -0.5, 0.09375)
    decay_rate = jnp.clip(jnp.exp(math.log(3.0) - 4.6051702 * jax.random.uniform(splits[8], (HEADS,), jnp.float32) ** levels(splits[8], (HEADS,), ((0, 16),), -0.2, 0.2)), 0.03, 3.0)
    decay_bias = jnp.clip(jax.random.uniform(splits[9], (HEADS,), jnp.float32, -1.0, 1.0) * levels(splits[9], (HEADS,), ((0, 16),), -0.4, 0.0), -1.0, 1.0)
    mix_gain = jnp.clip(1.0 + 0.18 * jax.random.normal(splits[10], (D,), jnp.float32), 0.1, 1.9)
    out_gain = jnp.clip(1.0 + 0.18 * jax.random.normal(splits[11], (HEAD_DIM,), jnp.float32), 0.1, 1.9)
    w_out = gaussian(splits[12], (HEADS * HEAD_DIM, D), (HEADS * HEAD_DIM) ** -0.5, 0.125, ((0, 16),))
    ffn_gain = jnp.clip(1.0 + 0.18 * jax.random.normal(splits[13], (D,), jnp.float32), 0.1, 1.9)
    w_up = gaussian(splits[14], (D, FF), D ** -0.5, 0.09375, ((0, 16), (1, 16)))
    w_down = gaussian(splits[15], (FF, D), FF ** -0.5, 0.046875, ((0, 16), (1, 16)))
    return {"tokens": tokens, "state": state, "w_query": w_query, "w_key": w_key, "w_value": w_value, "w_gate": w_gate, "w_decay": w_decay, "w_beta": w_beta, "decay_rate": decay_rate, "decay_bias": decay_bias, "mix_gain": mix_gain, "out_gain": out_gain, "w_out": w_out, "ffn_gain": ffn_gain, "w_up": w_up, "w_down": w_down}


EPS = 1e-06

def unit_norm(vector):
    return vector * lax.rsqrt(lax.optimization_barrier(jnp.sum(vector * vector, axis=-1, keepdims=True)) + EPS)

def reference(tokens, state, w_query, w_key, w_value, w_gate, w_decay, w_beta, decay_rate, decay_bias, mix_gain, out_gain, w_out, ffn_gain, w_up, w_down):
    rows = tokens.shape[0]
    tok_f = tokens.astype(jnp.float32)
    normed = (tok_f * lax.rsqrt(lax.optimization_barrier(jnp.mean(tok_f * tok_f, axis=-1, keepdims=True)) + EPS) * mix_gain).astype(jnp.bfloat16)
    query = jnp.dot(normed, w_query, preferred_element_type=jnp.float32).reshape(rows, HEADS, HEAD_DIM)
    key_proj = jnp.dot(normed, w_key, preferred_element_type=jnp.float32).reshape(rows, HEADS, HEAD_DIM)
    value = jnp.dot(normed, w_value, preferred_element_type=jnp.float32).reshape(rows, HEADS, HEAD_DIM)
    gate = jnp.dot(normed, w_gate, preferred_element_type=jnp.float32).reshape(rows, HEADS, HEAD_DIM)
    query = unit_norm(query) * HEAD_DIM ** (-0.5)
    key_proj = unit_norm(key_proj)
    pre_decay = jnp.dot(normed, w_decay, preferred_element_type=jnp.float32)
    decay = jnp.exp(-decay_rate * jax.nn.softplus(pre_decay + decay_bias))
    strength = jax.nn.sigmoid(jnp.dot(normed, w_beta, preferred_element_type=jnp.float32))
    matrix = state.reshape(rows, HEADS, HEAD_DIM, HEAD_DIM) * decay[:, :, None, None]
    recalled = jnp.einsum('bhk,bhkv->bhv', key_proj, matrix, precision=lax.Precision.HIGHEST)
    delta = (value - recalled) * strength[:, :, None]
    matrix = matrix + key_proj[:, :, :, None] * delta[:, :, None, :]
    head_out = jnp.einsum('bhk,bhkv->bhv', query, matrix, precision=lax.Precision.HIGHEST)
    head_out = head_out * lax.rsqrt(lax.optimization_barrier(jnp.mean(head_out * head_out, axis=-1, keepdims=True)) + EPS) * out_gain * jax.nn.silu(gate)
    head_out = head_out.reshape(rows, HEADS * HEAD_DIM).astype(jnp.bfloat16)
    resid = tok_f + jnp.dot(head_out, w_out, preferred_element_type=jnp.float32)
    ffn_in = (resid * lax.rsqrt(lax.optimization_barrier(jnp.mean(resid * resid, axis=-1, keepdims=True)) + EPS) * ffn_gain).astype(jnp.bfloat16)
    hidden = jnp.square(jax.nn.relu(jnp.dot(ffn_in, w_up, preferred_element_type=jnp.float32))).astype(jnp.bfloat16)
    mixed = (resid + jnp.dot(hidden, w_down, preferred_element_type=jnp.float32)).astype(jnp.bfloat16)
    return (mixed, matrix.reshape(rows, HEADS, HEAD_DIM * HEAD_DIM))
```

```python
import jax
import jax.numpy as jnp
from jax import lax
from jax.experimental import pallas as pl
from jax.experimental.pallas import tpu as pltpu
from jax.sharding import Mesh
from jax.sharding import PartitionSpec as P

D = 4096
HEAD_DIM = 64
EPS = 1e-06
F32 = jnp.float32
BF16 = jnp.bfloat16
TP = ("z", "c")


def attn_kernel(h0_ref, rate_ref, bias_ref, tok_ref, mg_ref, wq_ref, wk_ref, wv_ref, wg_ref, wd_ref, wb_ref, og_ref, st_hbm,
                ns_hbm, ho_ref, st, xn, kn, qn, vv, od, sem_in, sem_out):
    rows=tok_ref.shape[1]; width=tok_ref.shape[2]; parts=tok_ref.shape[0]
    nt=rows//8
    cin=pltpu.make_async_copy(st_hbm, st, sem_in); cin.start()
    ss=jnp.zeros((rows,1),F32)
    for t in range(parts):
        x=tok_ref[t].astype(F32); ss=ss+jnp.sum(x*x,axis=-1,keepdims=True)
    r=lax.rsqrt(ss/(parts*width)+EPS)
    for t in range(parts):
        xn[:,t*width:(t+1)*width]=(tok_ref[t].astype(F32)*r*mg_ref[t]).astype(BF16)
    x=xn[...]
    q=jnp.dot(x,wq_ref[...],preferred_element_type=F32)
    k=jnp.dot(x,wk_ref[...],preferred_element_type=F32)
    v=jnp.dot(x,wv_ref[...],preferred_element_type=F32)
    g=jnp.dot(x,wg_ref[...],preferred_element_type=F32)
    nt_dims=(((1,),(1,)),((),()))
    pd=lax.dot_general(x,wd_ref[...],nt_dims,preferred_element_type=F32)
    pb=lax.dot_general(x,wb_ref[...],nt_dims,preferred_element_type=F32)
    lane=lax.broadcasted_iota(jnp.int32,(rows,128),1)
    lo=lane<64
    def halves(a):
        s0=jnp.sum(jnp.where(lo,a,0.0),axis=-1,keepdims=True)
        s1=jnp.sum(jnp.where(lo,0.0,a),axis=-1,keepdims=True)
        return s0,s1
    def spread(s): return jnp.where(lo,s[0],s[1])
    qs=q*lax.rsqrt(spread(halves(q*q))+EPS)*(64**-0.5)
    ks=k*lax.rsqrt(spread(halves(k*k))+EPS)
    qn[...]=qs; kn[...]=ks; vv[...]=v
    kq=halves(qs*ks)
    hl=lax.broadcasted_iota(jnp.int32,pd.shape,1)
    h0=h0_ref[0]
    for h in range(2):
        sel=hl==h0+h
        d=jnp.sum(jnp.where(sel,pd,0.0),axis=-1,keepdims=True)+bias_ref[h]
        sp=jnp.maximum(d,0.0)+jnp.log1p(jnp.exp(-jnp.abs(d)))
        dec=jnp.exp(-rate_ref[h]*sp)
        b=jnp.sum(jnp.where(sel,pb,0.0),axis=-1,keepdims=True)
        stren=1.0/(1.0+jnp.exp(-b))
        od[h,0]=jnp.broadcast_to(dec,(rows,128))
        od[h,1]=jnp.broadcast_to(stren,(rows,128))
        od[h,2]=jnp.broadcast_to(kq[h],(rows,128))
    cin.wait()
    lane8=lax.broadcasted_iota(jnp.int32,(8,128),1)
    half8=lane8//64
    def pick(a,idx): return jnp.take_along_axis(a,idx,axis=1)
    def out_copy(bt): return pltpu.make_async_copy(st.at[pl.ds(bt*512,512),:],ns_hbm.at[pl.ds(bt*512,512),:],sem_out)
    def body(bt,_):
        r0=pl.multiple_of(bt*8,8)
        k8=kn[pl.ds(r0,8),:]; q8=qn[pl.ds(r0,8),:]; v8=vv[pl.ds(r0,8),:]
        for h in range(2):
            rec=jnp.zeros((8,128),F32); out=jnp.zeros((8,128),F32)
            S=[];K=[]
            for j in range(32):
                s=st[pl.ds(bt*512+2*j+h,8,stride=64),:]
                idx=half8+(h*64+2*j)
                ke=pick(k8,idx); qe=pick(q8,idx)
                rec=rec+s*ke; out=out+s*qe
                S.append(s);K.append(ke)
            rec=rec+pltpu.roll(rec,64,1); out=out+pltpu.roll(out,64,1)
            dec=od[h,0,pl.ds(r0,8),:]; stren=od[h,1,pl.ds(r0,8),:]; kq8=od[h,2,pl.ds(r0,8),:]
            vh=pick(v8,lane8-64*half8+h*64)
            delta=stren*(vh-dec*rec)
            od[h,3,pl.ds(r0,8),:]=dec*out+kq8*delta
            for j in range(32):
                st[pl.ds(bt*512+2*j+h,8,stride=64),:]=dec*S[j]+K[j]*delta
        @pl.when(bt>0)
        def _(): out_copy(bt-1).start()
        return 0
    lax.fori_loop(0,nt,body,0)
    o=jnp.where(lo,od[0,3],od[1,3])
    ms=spread(halves(o*o))*(1.0/64)
    ho=o*lax.rsqrt(ms+EPS)*og_ref[...]*(g/(1.0+jnp.exp(-g)))
    ho_ref[...]=ho.astype(BF16)
    out_copy(nt-1).start()
    def w(bt,_):
        out_copy(bt).wait(); return 0
    lax.fori_loop(0,nt,w,0)

def attn(tok,h0,wq,wk,wv,wg,wd,wb,rate,bias,mix_gain,out_gain,state):
    parts,rows,width=tok.shape
    mg=mix_gain.reshape(parts,1,width)
    og=jnp.tile(out_gain,2).reshape(1,128)
    heads=state.shape[1]
    st=state.reshape(rows,heads,32,128).transpose(0,2,1,3).reshape(rows*64,128)
    vm=pl.BlockSpec(memory_space=pltpu.VMEM); sm=pl.BlockSpec(memory_space=pltpu.SMEM); an=pl.BlockSpec(memory_space=pl.ANY)
    ns,ho=pl.pallas_call(attn_kernel,
        out_shape=(jax.ShapeDtypeStruct((rows*64,128),F32),jax.ShapeDtypeStruct((rows,128),BF16)),
        in_specs=[sm,sm,sm]+[vm]*9+[an],
        out_specs=(an,vm),
        scratch_shapes=[pltpu.VMEM((rows*64,128),F32),pltpu.VMEM((rows,parts*width),BF16)]+[pltpu.VMEM((rows,128),F32)]*3+[pltpu.VMEM((2,4,rows,128),F32),pltpu.SemaphoreType.DMA,pltpu.SemaphoreType.DMA],
        cost_estimate=pl.CostEstimate(flops=2*96*4096*600,bytes_accessed=12_000_000,transcendentals=50000),
        name="attn",
    )(h0,rate,bias,tok,mg,wq,wk,wv,wg,wd.T,wb.T,og,st)
    ns=ns.reshape(rows,32,heads,128).transpose(0,2,1,3).reshape(rows,heads,4096)
    return ns,ho


def shifted(array, by):
    length = lax.axis_size("z")
    return lax.ppermute(array, "z", [(i, (i + by) % length) for i in range(length)])


def other_core(array):
    return lax.ppermute(array, "c", [(0, 1), (1, 0)])


def add(*terms):
    total = terms[0].astype(F32)
    for term in terms[1:]:
        total = total + term.astype(F32)
    return total


def ring_sum(block):
    far = block(4)
    half = far.shape[0] // 2
    up = shifted(far[:half], 1)
    down = shifted(far[half:], -1)
    near, back = block(3), block(5)
    up = jnp.concatenate([add(near[:half], up).astype(BF16), near[half:]], 0)
    down = jnp.concatenate([back[:half], add(back[half:], down).astype(BF16)], 0)
    for step in (2, 1):
        up = add(block(step), shifted(up, 1)).astype(BF16)
        down = add(block(8 - step), shifted(down, -1)).astype(BF16)
    return add(block(0), shifted(up, 1), shifted(down, -1))


def ring_gather(block):
    parts = [None] * 8
    parts[0] = block
    rows = block.shape[0] // 2
    ahead = [block[:rows], block[rows:]]
    behind = [block[:rows], block[rows:]]
    for step in range(1, 4):
        behind = [shifted(piece, 1) for piece in behind]
        ahead = [shifted(piece, -1) for piece in ahead]
        parts[8 - step] = jnp.concatenate(behind, 0)
        parts[step] = jnp.concatenate(ahead, 0)
    parts[4] = jnp.concatenate([shifted(ahead[0], -1), shifted(behind[1], 1)], 0)
    return jnp.concatenate(parts, 0)


def local(
    tokens,
    state,
    w_query,
    w_key,
    w_value,
    w_gate,
    w_decay,
    w_beta,
    decay_rate,
    decay_bias,
    mix_gain,
    out_gain,
    w_out,
    ffn_gain,
    w_up,
    w_down,
):
    rows, width = tokens.shape
    z = lax.axis_index("z")
    c = lax.axis_index("c")
    tp = z * 2 + c
    hidden_half = w_up.shape[1] // 2
    up_mine = lax.dynamic_slice_in_dim(w_up, c * hidden_half, hidden_half, 1)
    up_other = other_core(lax.dynamic_slice_in_dim(w_up, (1 - c) * hidden_half, hidden_half, 1))
    down_mine = lax.dynamic_slice_in_dim(w_down, c * hidden_half, hidden_half, 0)
    down_other = other_core(lax.dynamic_slice_in_dim(w_down, (1 - c) * hidden_half, hidden_half, 0))

    everything = lax.all_gather(tokens, TP, axis=0, tiled=False)
    new_state, head_out = attn(
        everything, (tp * 2).reshape(1).astype(jnp.int32), w_query, w_key, w_value, w_gate, w_decay, w_beta,
        decay_rate, decay_bias, mix_gain, out_gain, state,
    )
    partial = jnp.dot(head_out, w_out, preferred_element_type=F32).astype(BF16)
    parts = jnp.moveaxis(partial.reshape(rows, -1, width), 1, 0)
    arrived = lax.all_to_all(parts, TP, 0, 0, tiled=True)
    resid = tokens.astype(F32) + arrived.astype(F32).sum(axis=0)
    gain = lax.dynamic_slice_in_dim(ffn_gain, tp * width, width, 0)
    squares = jnp.sum(resid * resid, axis=-1)
    all_squares = lax.all_to_all(jnp.broadcast_to(squares[None, None], (16, 1, rows)), TP, 0, 0, tiled=True)
    scaled = (resid * gain).astype(BF16)
    mine = lax.all_to_all(jnp.broadcast_to(scaled[None], (16, rows, width)), "kv", 0, 0, tiled=True)
    mine = mine.reshape(16 * rows, width)
    theirs = other_core(mine)
    up_part = (
        jnp.dot(mine, up_mine, preferred_element_type=F32) + jnp.dot(theirs, up_other, preferred_element_type=F32)
    ).astype(BF16)
    up_part = up_part.reshape(8, 2 * rows, hidden_half)

    def up_block(offset):
        return lax.dynamic_index_in_dim(up_part, lax.rem(z + offset, 8), 0, keepdims=False)

    hidden = jnp.square(jax.nn.relu(ring_sum(up_block))).astype(BF16)
    hidden = ring_gather(hidden)
    give = jnp.dot(hidden, down_other, preferred_element_type=F32).astype(BF16)
    took = other_core(give)
    down = (jnp.dot(hidden, down_mine, preferred_element_type=F32) + took.astype(F32)).astype(BF16)
    down = down.reshape(8, 2 * rows, width)
    down = lax.dynamic_slice_in_dim(jnp.concatenate([down, down], 0), lax.rem(8 - z, 8), 8, 0)
    down = lax.all_to_all(down.reshape(16, rows, width), "kv", 0, 0, tiled=True)
    down = down.astype(F32).sum(axis=0)
    square_scale = 1.0 / (jnp.sum(all_squares, axis=(0, 1)) / D + EPS)
    mixed = (resid + down * square_scale[:, None]).astype(BF16)
    return (mixed, new_state)


def solution(mesh):
    split = Mesh(mesh.devices.reshape(mesh.shape["kv"], 8, 2), ("kv", "z", "c"))
    placed = (
        P("kv", TP),
        P("kv", TP, None),
        P(None, TP),
        P(None, TP),
        P(None, TP),
        P(None, TP),
        P(),
        P(),
        P(TP),
        P(TP),
        P(),
        P(),
        P(TP, None),
        P(),
        P(TP, "kv"),
        P("kv", TP),
    )
    return jax.shard_map(
        local,
        mesh=split,
        in_specs=placed,
        out_specs=(P("kv", TP), P("kv", TP, None)),
        check_vma=False,
    )
```

```python
import jax
import jax.numpy as jnp
from jax import lax
from jax.experimental import pallas as pl
from jax.experimental.pallas import tpu as pltpu
from jax.sharding import Mesh
from jax.sharding import PartitionSpec as P

D = 4096
EPS = 1e-06
F32 = jnp.float32
BF16 = jnp.bfloat16
TP = ("z", "c")
KV = ("y", "x")
EVERYWHERE = ("y", "x", "z", "c")
PAD = 8


def attn_kernel(h0_ref, rate_ref, bias_ref, tok_ref, mg_ref, wq_hbm, wk_hbm, wv_hbm, wg_hbm, wd_hbm, wb_hbm, wo_hbm, og_ref, st_hbm,
                ns_hbm, keep_ref, give_ref, wo, w4, w2, st, xn, vv, od, ex, e2, sem_w, sem_in, sem_out):
    rows = tok_ref.shape[1]
    width = tok_ref.shape[2]
    parts = tok_ref.shape[0]
    nt = rows // 8
    loads = [pltpu.make_async_copy(src, w4.at[i], sem_w.at[i]) for i, src in enumerate((wq_hbm, wk_hbm, wv_hbm, wg_hbm))]
    loads += [pltpu.make_async_copy(src, w2.at[i], sem_w.at[4 + i]) for i, src in enumerate((wd_hbm, wb_hbm))]
    loads += [pltpu.make_async_copy(wo_hbm, wo, sem_w.at[6])]
    cin = pltpu.make_async_copy(st_hbm, st, sem_in)
    for i in (1, 0, 4, 5, 2):
        loads[i].start()
    cin.start()
    loads[3].start()
    loads[6].start()
    ei = lax.broadcasted_iota(jnp.int32, e2.shape, 0)
    ec = lax.broadcasted_iota(jnp.int32, e2.shape, 1)
    e2[...] = jnp.where((ei & 63) == (ec >> 6), 1.0, 0.0).astype(BF16)
    ss = jnp.zeros((rows, width), F32)
    for t in range(parts):
        x = tok_ref[t].astype(F32)
        ss = ss + x * x
    r = lax.rsqrt(jnp.sum(ss, axis=-1, keepdims=True) / (parts * width) + EPS)
    for t in range(parts):
        xn[:, t * width:(t + 1) * width] = (tok_ref[t].astype(F32) * r * mg_ref[t]).astype(BF16)
    x = xn[...]

    def proj(i):
        loads[i].wait()
        return jnp.dot(x, w4[i], preferred_element_type=F32)

    lane = lax.broadcasted_iota(jnp.int32, (rows, 128), 1)
    lo = lane < 64

    def halves(a):
        s0 = jnp.sum(jnp.where(lo, a, 0.0), axis=-1, keepdims=True)
        s1 = jnp.sum(jnp.where(lo, 0.0, a), axis=-1, keepdims=True)
        return s0, s1

    def spread(s):
        return jnp.where(lo, s[0], s[1])

    def expand(a, slot):
        hi = a.astype(BF16).astype(F32)
        low = a - hi
        for h in range(2):
            if h == 0:
                both = jnp.where(lo, hi, pltpu.roll(low, 64, 1))
            else:
                both = jnp.where(lo, pltpu.roll(hi, 64, 1), low)
            ex[slot + h] = jnp.dot(both.astype(BF16), e2[...], preferred_element_type=F32)

    k = proj(1)
    ks = k * lax.rsqrt(spread(halves(k * k)) + EPS)
    expand(ks, 0)
    q = proj(0)
    qs = q * lax.rsqrt(spread(halves(q * q)) + EPS) * (64 ** -0.5)
    expand(qs, 2)
    nt_dims = (((1,), (1,)), ((), ()))
    loads[4].wait()
    loads[5].wait()
    pd = lax.dot_general(x, w2[0], nt_dims, preferred_element_type=F32)
    pb = lax.dot_general(x, w2[1], nt_dims, preferred_element_type=F32)
    v = proj(2)
    vr = pltpu.roll(v, 64, 1)
    vv[0] = jnp.where(lo, v, vr)
    vv[1] = jnp.where(lo, vr, v)
    kq = halves(qs * ks)
    hl = lax.broadcasted_iota(jnp.int32, pd.shape, 1)
    h0 = h0_ref[0]
    for h in range(2):
        sel = hl == h0 + h
        d = jnp.sum(jnp.where(sel, pd, 0.0), axis=-1, keepdims=True) + bias_ref[h]
        sp = jnp.maximum(d, 0.0) + jnp.log1p(jnp.exp(-jnp.abs(d)))
        dec = jnp.exp(-rate_ref[h] * sp)
        b = jnp.sum(jnp.where(sel, pb, 0.0), axis=-1, keepdims=True)
        stren = 1.0 / (1.0 + jnp.exp(-b))
        od[h, 0] = jnp.broadcast_to(dec, (rows, 128))
        od[h, 1] = jnp.broadcast_to(stren, (rows, 128))
        od[h, 2] = jnp.broadcast_to(kq[h], (rows, 128))
    cin.wait()

    def out_copy(bt):
        return pltpu.make_async_copy(st.at[pl.ds(bt * 512, 512), :], ns_hbm.at[pl.ds(bt * 512, 512), :], sem_out)

    def body(bt, _):
        r0 = pl.multiple_of(bt * 8, 8)
        for h in range(2):
            rec = jnp.zeros((8, 128), F32)
            out = jnp.zeros((8, 128), F32)
            terms = []
            for j in range(32):
                s = st[pl.ds(bt * 512 + 2 * j + h, 8, stride=64), :]
                ke = ex[h, pl.ds(r0, 8), j * 128:(j + 1) * 128]
                qe = ex[2 + h, pl.ds(r0, 8), j * 128:(j + 1) * 128]
                rec = rec + s * ke
                out = out + s * qe
                terms.append(s)
            rec = rec + pltpu.roll(rec, 64, 1)
            out = out + pltpu.roll(out, 64, 1)
            dec = od[h, 0, pl.ds(r0, 8), :]
            stren = od[h, 1, pl.ds(r0, 8), :]
            kq8 = od[h, 2, pl.ds(r0, 8), :]
            delta = stren * (vv[h, pl.ds(r0, 8), :] - dec * rec)
            od[h, 3, pl.ds(r0, 8), :] = dec * out + kq8 * delta
            for j in range(32):
                ke = ex[h, pl.ds(r0, 8), j * 128:(j + 1) * 128]
                st[pl.ds(bt * 512 + 2 * j + h, 8, stride=64), :] = dec * terms[j] + ke * delta

        @pl.when(bt > 0)
        def _():
            out_copy(bt - 1).start()

        return 0

    lax.fori_loop(0, nt, body, 0)
    g = proj(3)
    o = jnp.where(lo, od[0, 3], od[1, 3])
    ms = spread(halves(o * o)) * (1.0 / 64)
    gain = jnp.concatenate([og_ref[...], og_ref[...]], axis=1)
    ho = o * lax.rsqrt(ms + EPS) * gain * (g / (1.0 + jnp.exp(-g)))
    head_out = ho.astype(BF16)
    loads[6].wait()
    core = h0_ref[1]
    for i in range(keep_ref.shape[0]):
        for ref, side in ((give_ref, 1 - core), (keep_ref, core)):
            cols = wo[:, pl.ds(pl.multiple_of((2 * i + side) * width, width), width)]
            ref[i] = jnp.dot(head_out, cols, preferred_element_type=F32).astype(BF16)
    out_copy(nt - 1).start()

    def finish(bt, _):
        out_copy(bt).wait()
        return 0

    lax.fori_loop(0, nt, finish, 0)


def attn(tok, h0, wq, wk, wv, wg, wd, wb, wo, rate, bias, mix_gain, out_gain, state):
    parts, rows, width = tok.shape
    mg = mix_gain.reshape(parts, 1, width)
    heads = state.shape[1]
    st = state.reshape(rows, heads, 32, 128).transpose(0, 2, 1, 3).reshape(rows * 64, 128)
    vm = pl.BlockSpec(memory_space=pltpu.VMEM)
    sm = pl.BlockSpec(memory_space=pltpu.SMEM)
    an = pl.BlockSpec(memory_space=pl.ANY)
    ns, keep, give = pl.pallas_call(
        attn_kernel,
        out_shape=(jax.ShapeDtypeStruct((rows * 64, 128), F32), jax.ShapeDtypeStruct((8, rows, width), BF16), jax.ShapeDtypeStruct((8, rows, width), BF16)),
        in_specs=[sm, sm, sm, vm, vm] + [an] * 7 + [vm, an],
        out_specs=(an, vm, vm),
        scratch_shapes=[
            pltpu.VMEM(wo.shape, BF16),
            pltpu.VMEM((4,) + wq.shape, BF16),
            pltpu.VMEM((2,) + wd.shape[::-1], BF16),
            pltpu.VMEM((rows * 64, 128), F32),
            pltpu.VMEM((rows, parts * width), BF16),
            pltpu.VMEM((2, rows, 128), F32),
            pltpu.VMEM((2, 4, rows, 128), F32),
            pltpu.VMEM((4, rows, 4096), F32),
            pltpu.VMEM((128, 4096), BF16),
            pltpu.SemaphoreType.DMA((7,)),
            pltpu.SemaphoreType.DMA,
            pltpu.SemaphoreType.DMA,
        ],
        compiler_params=pltpu.CompilerParams(vmem_limit_bytes=56 * 1024 * 1024),
        cost_estimate=pl.CostEstimate(flops=2 * 96 * 4096 * 600, bytes_accessed=12_000_000, transcendentals=50000),
        name="attn",
    )(h0, rate, bias, tok, mg, wq, wk, wv, wg, wd.T, wb.T, wo, out_gain.reshape(1, 64), st)
    ns = ns.reshape(rows, 32, heads, 128).transpose(0, 2, 1, 3).reshape(rows, heads, 4096)
    return ns, keep, give


VM = pl.BlockSpec(memory_space=pltpu.VMEM)
SM = pl.BlockSpec(memory_space=pltpu.SMEM)


def shifted(array, by, axis="z"):
    length = lax.axis_size(axis)
    return lax.ppermute(array, axis, [(i, (i + by) % length) for i in range(length)])


def other_core(array):
    return lax.ppermute(array, "c", [(0, 1), (1, 0)])


def out_kernel(tok_ref, gain_ref, parts_ref, resid_ref, send_ref):
    rows, width = tok_ref.shape
    acc = tok_ref[...].astype(F32)
    for i in range(parts_ref.shape[0]):
        acc = acc + parts_ref[i].astype(F32)
    resid_ref[...] = acc
    squares = jnp.sum(acc * acc, axis=-1, keepdims=True)
    eye = lax.broadcasted_iota(jnp.int32, (rows, 128), 0) == lax.broadcasted_iota(jnp.int32, (rows, 128), 1)
    flat = jnp.sum(jnp.where(eye, squares, 0.0), axis=0, keepdims=True)
    scaled = (acc * gain_ref[...]).astype(BF16)
    extra = jnp.broadcast_to(flat, (PAD, 128)).astype(BF16)
    blank = jnp.zeros((PAD, width - 128), BF16)
    for i in range(send_ref.shape[0]):
        send_ref[i, :rows, :] = scaled
        send_ref[i, rows:, :128] = extra
        send_ref[i, rows:, 128:] = blank


def residual(tokens, gain, parts):
    rows, width = tokens.shape
    return pl.pallas_call(
        out_kernel,
        out_shape=(jax.ShapeDtypeStruct((rows, width), F32), jax.ShapeDtypeStruct((16, rows + PAD, width), BF16)),
        in_specs=[VM] * 3,
        out_specs=(VM, VM),
        compiler_params=pltpu.CompilerParams(vmem_limit_bytes=16 * 1024 * 1024),
        cost_estimate=pl.CostEstimate(flops=1_000_000, bytes_accessed=2_000_000, transcendentals=0),
        name="out",
    )(tokens, gain, parts)


def up_kernel(z_ref, mine_ref, other_ref, wm_ref, wo_ref, *outs):
    rows = mine_ref.shape[1] - PAD
    width = mine_ref.shape[2]
    for o in (4, 3, 5, 2, 6, 1, 7, 0):
        at = (z_ref[0] + o) & 7
        own = mine_ref[pl.ds(2 * at, 2)]
        his = other_ref[pl.ds(2 * at, 2)]
        outs[o][: 2 * rows, :] = (
            jnp.dot(own[:, :rows].reshape(2 * rows, width), wm_ref[...], preferred_element_type=F32)
            + jnp.dot(his[:, :rows].reshape(2 * rows, width), wo_ref[...], preferred_element_type=F32)
        ).astype(BF16)
        squares = own[:, rows:, :128].astype(F32) + his[:, rows:, :128].astype(F32)
        outs[o][2 * rows :, :128] = squares[0].astype(BF16)
        outs[o][2 * rows :, 128:256] = squares[1].astype(BF16)
        outs[o][2 * rows :, 256:] = jnp.zeros((PAD, outs[o].shape[1] - 256), BF16)


def up_product(z, mine, other, w_mine, w_other):
    rows = mine.shape[1] - PAD
    return pl.pallas_call(
        up_kernel,
        out_shape=tuple(jax.ShapeDtypeStruct((2 * rows + PAD, w_mine.shape[1]), BF16) for _ in range(8)),
        in_specs=[SM] + [VM] * 4,
        out_specs=tuple([VM] * 8),
        compiler_params=pltpu.CompilerParams(vmem_limit_bytes=24 * 1024 * 1024),
        cost_estimate=pl.CostEstimate(flops=2 * 1536 * 512 * 512, bytes_accessed=4_000_000, transcendentals=0),
        name="up",
    )(z.reshape(1), mine, other, w_mine, w_other)


def hidden_kernel(a_ref, b_ref, c_ref, out_ref):
    total = a_ref[...].astype(F32) + b_ref[...].astype(F32) + c_ref[...].astype(F32)
    both = out_ref.shape[0]
    rows = both // 2
    eye = lax.broadcasted_iota(jnp.int32, (rows, 128), 0) == lax.broadcasted_iota(jnp.int32, (rows, 128), 1)
    for b in range(2):
        flat = total[both : both + 1, b * 128 : (b + 1) * 128]
        squares = jnp.sum(jnp.where(eye, flat, 0.0), axis=1, keepdims=True)
        up = jnp.maximum(total[b * rows : (b + 1) * rows], 0.0)
        out_ref[b * rows : (b + 1) * rows, :] = (up * up / (squares / D + EPS)).astype(BF16)


def finish_hidden(first, second, third):
    return pl.pallas_call(
        hidden_kernel,
        out_shape=jax.ShapeDtypeStruct((first.shape[0] - PAD, first.shape[1]), BF16),
        in_specs=[VM] * 3,
        out_specs=VM,
        compiler_params=pltpu.CompilerParams(vmem_limit_bytes=16 * 1024 * 1024),
        cost_estimate=pl.CostEstimate(flops=1_000_000, bytes_accessed=800_000, transcendentals=0),
        name="hidden",
    )(first, second, third)


def add(one, two):
    return (one.astype(F32) + two.astype(F32)).astype(BF16)


def ring_sum(blocks):
    ahead = blocks[4]
    back = blocks[5]
    ahead = add(blocks[3], shifted(ahead, 1))
    for step in (2, 1):
        ahead = add(blocks[step], shifted(ahead, 1))
        back = add(blocks[8 - step], shifted(back, -1))
    return blocks[0], shifted(ahead, 1), shifted(back, -1)


def ring_gather(block, *after):
    parts = [None] * 8
    parts[0] = block
    half = block.shape[0] // 2
    ahead = behind = block
    for step in range(1, 4):
        if after[step - 1] is not None:
            ahead, behind, _ = lax.optimization_barrier((ahead, behind, after[step - 1]))
        behind = shifted(behind, 1)
        ahead = shifted(ahead, -1)
        parts[8 - step] = behind
        parts[step] = ahead
    ahead, behind, _ = lax.optimization_barrier((ahead, behind, after[3]))
    low = shifted(ahead[:half], -1)
    high = shifted(behind[half:], 1)
    parts[4:5] = [low, high]
    return parts


def down_kernel(c_ref, mine_ref, other_ref, *refs):
    weights, out_ref = refs[:-1], refs[-1]
    rows = out_ref.shape[1]
    half = mine_ref.shape[1]
    flip = jnp.broadcast_to(c_ref[0], mine_ref.shape) > 0
    mine = mine_ref[...].astype(F32)
    other = other_ref[...].astype(F32)
    low = jnp.where(flip, other, mine).astype(BF16)
    high = jnp.where(flip, mine, other).astype(BF16)
    for o in range(8):
        if o == 4:
            top, bottom = weights[4][...], weights[5][...]
        else:
            ref = weights[o] if o < 4 else weights[o + 1]
            top, bottom = ref[:half, :], ref[half:, :]
        out = jnp.dot(low, top, preferred_element_type=F32) + jnp.dot(high, bottom, preferred_element_type=F32)
        out_ref[2 * o] = out[:rows].astype(BF16)
        out_ref[2 * o + 1] = out[rows:].astype(BF16)


def down_product(c, mine, other, weights):
    rows = mine.shape[0] // 2
    width = weights[0].shape[1]
    return pl.pallas_call(
        down_kernel,
        out_shape=jax.ShapeDtypeStruct((16, rows, width), BF16),
        in_specs=[SM] + [VM] * 11,
        out_specs=VM,
        compiler_params=pltpu.CompilerParams(vmem_limit_bytes=24 * 1024 * 1024),
        cost_estimate=pl.CostEstimate(flops=2 * 192 * 1024 * 2048, bytes_accessed=6_000_000, transcendentals=0),
        name="down",
    )(c.reshape(1), mine, other, *weights)


def layer(
    tokens,
    state,
    w_query,
    w_key,
    w_value,
    w_gate,
    w_decay,
    w_beta,
    decay_rate,
    decay_bias,
    mix_gain,
    out_gain,
    w_out,
    ffn_gain,
    w_up,
    w_down,
):
    _, width = tokens.shape
    _, _, z, c = (lax.axis_index(axis).astype(jnp.int32) for axis in EVERYWHERE)
    tp = z * 2 + c
    half = w_up.shape[1] // 2
    everything = lax.all_gather(tokens, TP, axis=0, tiled=False)
    up_mine = lax.dynamic_slice_in_dim(w_up, c * half, half, 1)
    up_other = other_core(lax.dynamic_slice_in_dim(w_up, (1 - c) * half, half, 1))
    gain = lax.dynamic_slice_in_dim(ffn_gain, tp * width, width, 0).reshape(1, width)
    everything, up_other = lax.optimization_barrier((everything, up_other))
    new_state, keep, give = attn(
        everything, jnp.stack([tp * 2, c]), w_query, w_key, w_value, w_gate, w_decay, w_beta, w_out,
        decay_rate, decay_bias, mix_gain, out_gain, state,
    )
    took = other_core(give)
    parts = lax.all_to_all(add(keep, took), "z", 0, 0, tiled=True)
    resid, send = residual(tokens, gain, parts)
    mine = lax.all_to_all(send, KV, 0, 0, tiled=True)
    theirs = other_core(mine)
    blocks = up_product(z, mine, theirs, up_mine, up_other)
    down_weights = ring_gather(w_down, None, everything, parts, mine)
    hidden = finish_hidden(*ring_sum(blocks))
    down = down_product(c, hidden, other_core(hidden), down_weights)
    down = lax.all_to_all(down, KV, 0, 0, tiled=True)
    down = down.astype(F32).sum(axis=0).astype(BF16)
    routes = [
        (((2 * o + b) * 8 + s) * 2 + k, ((2 * s + b) * 8 + (s + o) % 8) * 2 + k)
        for o in range(8) for b in range(2) for s in range(8) for k in range(2)
    ]
    down = lax.ppermute(down, EVERYWHERE, routes)
    mixed = (resid + down.astype(F32)).astype(BF16)
    return (mixed, new_state)


def solution(mesh):
    split = Mesh(mesh.devices.reshape(4, 4, 8, 2), EVERYWHERE)
    placed = (
        P(KV, TP),
        P(KV, TP, None),
        P(None, TP),
        P(None, TP),
        P(None, TP),
        P(None, TP),
        P(),
        P(),
        P(TP),
        P(TP),
        P(),
        P(),
        P(TP, None),
        P(),
        P(TP, KV),
        P(KV, TP),
    )
    return jax.shard_map(
        layer,
        mesh=split,
        in_specs=placed,
        out_specs=(P(KV, TP), P(KV, TP, None)),
        check_vma=False,
    )
```

```python
import functools

import jax
import jax.numpy as jnp
from jax import lax
from jax.experimental import pallas as pl
from jax.experimental.pallas import tpu as pltpu
from jax.sharding import Mesh
from jax.sharding import PartitionSpec as P

D = 4096
EPS = 1e-06
F32 = jnp.float32
BF16 = jnp.bfloat16
TP = ("z", "c")
KV = ("y", "x")
EVERYWHERE = ("y", "x", "z", "c")
PAD = 8


def attn_kernel(h0_ref, core_ref, rate_ref, bias_ref, tok_ref, mg_ref, wq_hbm, wk_hbm, wv_hbm, wg_hbm, wd_hbm, wb_hbm, wo_hbm, og_ref, st_hbm,
                ns_hbm, keep_ref, give_ref, wo, w4, w2, st, xn, vv, od, ex, e2, sem_w, sem_in, sem_out):
    rows = tok_ref.shape[1]
    width = tok_ref.shape[2]
    parts = tok_ref.shape[0]
    nt = rows // 8
    loads = [pltpu.make_async_copy(src, w4.at[i], sem_w.at[i]) for i, src in enumerate((wq_hbm, wk_hbm, wv_hbm, wg_hbm))]
    loads += [pltpu.make_async_copy(src, w2.at[i], sem_w.at[4 + i]) for i, src in enumerate((wd_hbm, wb_hbm))]
    loads += [pltpu.make_async_copy(wo_hbm, wo, sem_w.at[6])]
    cin = pltpu.make_async_copy(st_hbm, st, sem_in)
    for i in (1, 0, 4, 5, 2):
        loads[i].start()
    cin.start()
    loads[3].start()
    loads[6].start()
    ei = lax.broadcasted_iota(jnp.int32, e2.shape, 0)
    ec = lax.broadcasted_iota(jnp.int32, e2.shape, 1)
    e2[...] = jnp.where((ei & 63) == (ec >> 6), 1.0, 0.0).astype(BF16)
    ss = jnp.zeros((rows, width), F32)
    for t in range(parts):
        x = tok_ref[t].astype(F32)
        ss = ss + x * x
    r = lax.rsqrt(jnp.sum(ss, axis=-1, keepdims=True) / (parts * width) + EPS)
    for t in range(parts):
        xn[:, t * width:(t + 1) * width] = (tok_ref[t].astype(F32) * r * mg_ref[t]).astype(BF16)
    x = xn[...]

    def proj(i):
        loads[i].wait()
        return jnp.dot(x, w4[i], preferred_element_type=F32)

    lane = lax.broadcasted_iota(jnp.int32, (rows, 128), 1)
    lo = lane < 64

    def halves(a):
        s0 = jnp.sum(jnp.where(lo, a, 0.0), axis=-1, keepdims=True)
        s1 = jnp.sum(jnp.where(lo, 0.0, a), axis=-1, keepdims=True)
        return s0, s1

    def spread(s):
        return jnp.where(lo, s[0], s[1])

    def expand(a, slot):
        hi = a.astype(BF16).astype(F32)
        low = a - hi
        for h in range(2):
            if h == 0:
                both = jnp.where(lo, hi, pltpu.roll(low, 64, 1))
            else:
                both = jnp.where(lo, pltpu.roll(hi, 64, 1), low)
            ex[slot + h] = jnp.dot(both.astype(BF16), e2[...], preferred_element_type=F32)

    k = proj(1)
    ks = k * lax.rsqrt(spread(halves(k * k)) + EPS)
    expand(ks, 0)
    q = proj(0)
    qs = q * lax.rsqrt(spread(halves(q * q)) + EPS) * (64 ** -0.5)
    expand(qs, 2)
    nt_dims = (((1,), (1,)), ((), ()))
    loads[4].wait()
    loads[5].wait()
    pd = lax.dot_general(x, w2[0], nt_dims, preferred_element_type=F32)
    pb = lax.dot_general(x, w2[1], nt_dims, preferred_element_type=F32)
    v = proj(2)
    vr = pltpu.roll(v, 64, 1)
    vv[0] = jnp.where(lo, v, vr)
    vv[1] = jnp.where(lo, vr, v)
    kq = halves(qs * ks)
    hl = lax.broadcasted_iota(jnp.int32, pd.shape, 1)
    h0 = h0_ref[0]
    for h in range(2):
        sel = hl == h0 + h
        d = jnp.sum(jnp.where(sel, pd, 0.0), axis=-1, keepdims=True) + bias_ref[h]
        sp = jnp.maximum(d, 0.0) + jnp.log1p(jnp.exp(-jnp.abs(d)))
        dec = jnp.exp(-rate_ref[h] * sp)
        b = jnp.sum(jnp.where(sel, pb, 0.0), axis=-1, keepdims=True)
        stren = 1.0 / (1.0 + jnp.exp(-b))
        od[h, 0] = jnp.broadcast_to(dec, (rows, 128))
        od[h, 1] = jnp.broadcast_to(stren, (rows, 128))
        od[h, 2] = jnp.broadcast_to(kq[h], (rows, 128))
    cin.wait()

    def out_copy(bt):
        return pltpu.make_async_copy(st.at[pl.ds(bt * 512, 512), :], ns_hbm.at[pl.ds(bt * 512, 512), :], sem_out)

    def body(bt, _):
        r0 = pl.multiple_of(bt * 8, 8)
        for h in range(2):
            rec = jnp.zeros((8, 128), F32)
            out = jnp.zeros((8, 128), F32)
            terms = []
            for j in range(32):
                s = st[pl.ds(bt * 512 + 2 * j + h, 8, stride=64), :]
                ke = ex[h, pl.ds(r0, 8), j * 128:(j + 1) * 128]
                qe = ex[2 + h, pl.ds(r0, 8), j * 128:(j + 1) * 128]
                rec = rec + s * ke
                out = out + s * qe
                terms.append(s)
            rec = rec + pltpu.roll(rec, 64, 1)
            out = out + pltpu.roll(out, 64, 1)
            dec = od[h, 0, pl.ds(r0, 8), :]
            stren = od[h, 1, pl.ds(r0, 8), :]
            kq8 = od[h, 2, pl.ds(r0, 8), :]
            delta = stren * (vv[h, pl.ds(r0, 8), :] - dec * rec)
            od[h, 3, pl.ds(r0, 8), :] = dec * out + kq8 * delta
            for j in range(32):
                ke = ex[h, pl.ds(r0, 8), j * 128:(j + 1) * 128]
                st[pl.ds(bt * 512 + 2 * j + h, 8, stride=64), :] = dec * terms[j] + ke * delta

        @pl.when(bt > 0)
        def _():
            out_copy(bt - 1).start()

        return 0

    lax.fori_loop(0, nt, body, 0)
    g = proj(3)
    o = jnp.where(lo, od[0, 3], od[1, 3])
    ms = spread(halves(o * o)) * (1.0 / 64)
    gain = jnp.concatenate([og_ref[...], og_ref[...]], axis=1)
    ho = o * lax.rsqrt(ms + EPS) * gain * (g / (1.0 + jnp.exp(-g)))
    head_out = ho.astype(BF16)
    loads[6].wait()
    core = core_ref[0]
    for i in range(keep_ref.shape[0]):
        for ref, side in ((give_ref, 1 - core), (keep_ref, core)):
            cols = wo[:, pl.ds(pl.multiple_of((2 * i + side) * width, width), width)]
            ref[i] = jnp.dot(head_out, cols, preferred_element_type=F32).astype(BF16)
    out_copy(nt - 1).start()

    def finish(bt, _):
        out_copy(bt).wait()
        return 0

    lax.fori_loop(0, nt, finish, 0)


def attn(tok, h0, core, wq, wk, wv, wg, wd, wb, wo, rate, bias, mix_gain, out_gain, state):
    parts, rows, width = tok.shape
    mg = mix_gain.reshape(parts, 1, width)
    heads = state.shape[1]
    st = state.reshape(rows, heads, 32, 128).transpose(0, 2, 1, 3).reshape(rows * 64, 128)
    vm = pl.BlockSpec(memory_space=pltpu.VMEM)
    sm = pl.BlockSpec(memory_space=pltpu.SMEM)
    an = pl.BlockSpec(memory_space=pl.ANY)
    ns, keep, give = pl.pallas_call(
        attn_kernel,
        out_shape=(jax.ShapeDtypeStruct((rows * 64, 128), F32), jax.ShapeDtypeStruct((8, rows, width), BF16), jax.ShapeDtypeStruct((8, rows, width), BF16)),
        in_specs=[sm, sm, sm, sm, vm, vm] + [an] * 7 + [vm, an],
        out_specs=(an, vm, vm),
        scratch_shapes=[
            pltpu.VMEM(wo.shape, BF16),
            pltpu.VMEM((4,) + wq.shape, BF16),
            pltpu.VMEM((2,) + wd.shape[::-1], BF16),
            pltpu.VMEM((rows * 64, 128), F32),
            pltpu.VMEM((rows, parts * width), BF16),
            pltpu.VMEM((2, rows, 128), F32),
            pltpu.VMEM((2, 4, rows, 128), F32),
            pltpu.VMEM((4, rows, 4096), F32),
            pltpu.VMEM((128, 4096), BF16),
            pltpu.SemaphoreType.DMA((7,)),
            pltpu.SemaphoreType.DMA,
            pltpu.SemaphoreType.DMA,
        ],
        compiler_params=pltpu.CompilerParams(vmem_limit_bytes=56 * 1024 * 1024),
        cost_estimate=pl.CostEstimate(flops=2 * 96 * 4096 * 600, bytes_accessed=12_000_000, transcendentals=50000),
        name="attn",
    )(h0, core, rate, bias, tok, mg, wq, wk, wv, wg, wd.T, wb.T, wo, out_gain.reshape(1, 64), st)
    ns = ns.reshape(rows, 32, heads, 128).transpose(0, 2, 1, 3).reshape(rows, heads, 4096)
    return ns, keep, give


VM = pl.BlockSpec(memory_space=pltpu.VMEM)
SM = pl.BlockSpec(memory_space=pltpu.SMEM)


def shifted(array, by, axis="z"):
    length = lax.axis_size(axis)
    return lax.ppermute(array, axis, [(i, (i + by) % length) for i in range(length)])


def other_core(array):
    return lax.ppermute(array, "c", [(0, 1), (1, 0)])


def out_kernel(tok_ref, gain_ref, parts_ref, resid_ref, send_ref):
    rows, width = tok_ref.shape
    acc = tok_ref[...].astype(F32)
    for i in range(parts_ref.shape[0]):
        acc = acc + parts_ref[i].astype(F32)
    resid_ref[...] = acc
    squares = jnp.sum(acc * acc, axis=-1, keepdims=True)
    eye = lax.broadcasted_iota(jnp.int32, (rows, 128), 0) == lax.broadcasted_iota(jnp.int32, (rows, 128), 1)
    flat = jnp.sum(jnp.where(eye, squares, 0.0), axis=0, keepdims=True)
    scaled = (acc * gain_ref[...]).astype(BF16)
    extra = jnp.broadcast_to(flat, (PAD, 128)).astype(BF16)
    blank = jnp.zeros((PAD, width - 128), BF16)
    for i in range(send_ref.shape[0]):
        send_ref[i, :rows, :] = scaled
        send_ref[i, rows:, :128] = extra
        send_ref[i, rows:, 128:] = blank


def residual(tokens, gain, parts):
    rows, width = tokens.shape
    return pl.pallas_call(
        out_kernel,
        out_shape=(jax.ShapeDtypeStruct((rows, width), F32), jax.ShapeDtypeStruct((16, rows + PAD, width), BF16)),
        in_specs=[VM] * 3,
        out_specs=(VM, VM),
        compiler_params=pltpu.CompilerParams(vmem_limit_bytes=16 * 1024 * 1024),
        cost_estimate=pl.CostEstimate(flops=1_000_000, bytes_accessed=2_000_000, transcendentals=0),
        name="out",
    )(tokens, gain, parts)


def up_kernel(z_ref, mine_ref, other_ref, wm_ref, wo_ref, *outs):
    rows = mine_ref.shape[1] - PAD
    width = mine_ref.shape[2]
    for o in (4, 3, 5, 2, 6, 1, 7, 0):
        at = (z_ref[0] + o) & 7
        own = mine_ref[pl.ds(2 * at, 2)]
        his = other_ref[pl.ds(2 * at, 2)]
        product = (
            jnp.dot(own[:, :rows].reshape(2 * rows, width), wm_ref[...], preferred_element_type=F32)
            + jnp.dot(his[:, :rows].reshape(2 * rows, width), wo_ref[...], preferred_element_type=F32)
        ).astype(BF16)
        squares = own[:, rows:, :128].astype(F32) + his[:, rows:, :128].astype(F32)
        side = product.shape[1] // 2
        left, right = outs[o], outs[o]
        shift = side
        if o == 4:
            right, shift = outs[8], 0
        left[: 2 * rows, :side] = product[:, :side]
        left[2 * rows :, :128] = squares[0].astype(BF16)
        left[2 * rows :, 128:256] = squares[1].astype(BF16)
        right[: 2 * rows, shift : shift + side] = product[:, side:]
        right[2 * rows :, shift : shift + side] = jnp.zeros((PAD, side), BF16)


def up_product(z, mine, other, w_mine, w_other):
    rows = mine.shape[1] - PAD
    return pl.pallas_call(
        up_kernel,
        out_shape=tuple(
            jax.ShapeDtypeStruct((2 * rows + PAD, w_mine.shape[1] // (2 if o in (4, 8) else 1)), BF16) for o in range(9)
        ),
        in_specs=[SM] + [VM] * 4,
        out_specs=tuple([VM] * 9),
        compiler_params=pltpu.CompilerParams(vmem_limit_bytes=24 * 1024 * 1024),
        cost_estimate=pl.CostEstimate(flops=2 * 1536 * 512 * 512, bytes_accessed=4_000_000, transcendentals=0),
        name="up",
    )(z.reshape(1), mine, other, w_mine, w_other)


def hidden_kernel(a_ref, b_ref, c_ref, out_ref):
    total = a_ref[...].astype(F32) + b_ref[...].astype(F32) + c_ref[...].astype(F32)
    both = out_ref.shape[0]
    rows = both // 2
    eye = lax.broadcasted_iota(jnp.int32, (rows, 128), 0) == lax.broadcasted_iota(jnp.int32, (rows, 128), 1)
    for b in range(2):
        flat = total[both : both + 1, b * 128 : (b + 1) * 128]
        squares = jnp.sum(jnp.where(eye, flat, 0.0), axis=1, keepdims=True)
        up = jnp.maximum(total[b * rows : (b + 1) * rows], 0.0)
        out_ref[b * rows : (b + 1) * rows, :] = (up * up / (squares / D + EPS)).astype(BF16)


def finish_hidden(first, second, third):
    return pl.pallas_call(
        hidden_kernel,
        out_shape=jax.ShapeDtypeStruct((first.shape[0] - PAD, first.shape[1]), BF16),
        in_specs=[VM] * 3,
        out_specs=VM,
        compiler_params=pltpu.CompilerParams(vmem_limit_bytes=16 * 1024 * 1024),
        cost_estimate=pl.CostEstimate(flops=1_000_000, bytes_accessed=800_000, transcendentals=0),
        name="hidden",
    )(first, second, third)


def pair_kernel(one_ref, two_ref, out_ref):
    out_ref[...] = (one_ref[...].astype(F32) + two_ref[...].astype(F32)).astype(BF16)


def pair_sum(one, two):
    return pl.pallas_call(
        pair_kernel,
        out_shape=jax.ShapeDtypeStruct(one.shape, BF16),
        in_specs=[VM] * 2,
        out_specs=VM,
        compiler_params=pltpu.CompilerParams(vmem_limit_bytes=16 * 1024 * 1024),
        cost_estimate=pl.CostEstimate(flops=1_000_000, bytes_accessed=1_000_000, transcendentals=0),
        name="pair",
    )(one, two)


def add(one, two):
    return (one.astype(F32) + two.astype(F32)).astype(BF16)


def half_kernel(start, full_ref, part_ref, out_ref):
    out_ref[...] = full_ref[...]
    cols = slice(start, start + part_ref.shape[1])
    out_ref[:, cols] = (full_ref[:, cols].astype(F32) + part_ref[...].astype(F32)).astype(BF16)


def half_sum(full, part, start):
    return pl.pallas_call(
        functools.partial(half_kernel, start),
        out_shape=jax.ShapeDtypeStruct(full.shape, BF16),
        in_specs=[VM] * 2,
        out_specs=VM,
        compiler_params=pltpu.CompilerParams(vmem_limit_bytes=8 * 1024 * 1024),
        cost_estimate=pl.CostEstimate(flops=100_000, bytes_accessed=500_000, transcendentals=0),
        name="half",
    )(full, part)


def ring_sum(blocks):
    ahead = shifted(blocks[4], 1)
    back = shifted(blocks[8], -1)
    ahead = half_sum(blocks[3], ahead, 0)
    ahead = shifted(ahead, 1)
    back = half_sum(blocks[5], back, blocks[4].shape[1])
    back = shifted(back, -1)
    for step in (2, 1):
        ahead = add(blocks[step], ahead)
        ahead = shifted(ahead, 1)
        back = add(blocks[8 - step], back)
        back = shifted(back, -1)
    return blocks[0], ahead, back


def tied(array, *others):
    return lax.optimization_barrier((array,) + others)[0]


def ring_gather(block, *after):
    parts = [None] * 8
    parts[0] = block
    half = block.shape[0] // 2
    ahead = behind = block
    for step in range(1, 4):
        if after[step - 1] is not None:
            ahead, behind, _ = lax.optimization_barrier((ahead, behind, after[step - 1]))
        behind = shifted(behind, 1)
        ahead = shifted(ahead, -1)
        parts[8 - step] = behind
        parts[step] = ahead
    ahead, behind, _ = lax.optimization_barrier((ahead, behind, after[3]))
    low = shifted(ahead[:half], -1)
    high = shifted(behind[half:], 1)
    parts[4:5] = [low, high]
    return parts


def down_kernel(z_ref, c_ref, mine_ref, other_ref, *refs):
    weights, out_ref = refs[:-1], refs[-1]
    rows = out_ref.shape[1]
    half = mine_ref.shape[1]
    flip = jnp.broadcast_to(c_ref[0], mine_ref.shape) > 0
    mine = mine_ref[...].astype(F32)
    other = other_ref[...].astype(F32)
    low = jnp.where(flip, other, mine).astype(BF16)
    high = jnp.where(flip, mine, other).astype(BF16)
    for o in range(8):
        if o == 4:
            top, bottom = weights[4][...], weights[5][...]
        else:
            ref = weights[o] if o < 4 else weights[o + 1]
            top, bottom = ref[:half, :], ref[half:, :]
        out = jnp.dot(low, top, preferred_element_type=F32) + jnp.dot(high, bottom, preferred_element_type=F32)
        at = (o + 2 * z_ref[0]) & 7
        out_ref[2 * at] = out[:rows].astype(BF16)
        out_ref[2 * at + 1] = out[rows:].astype(BF16)


def down_product(z, c, mine, other, weights):
    rows = mine.shape[0] // 2
    width = weights[0].shape[1]
    return pl.pallas_call(
        down_kernel,
        out_shape=jax.ShapeDtypeStruct((16, rows, width), BF16),
        in_specs=[SM, SM] + [VM] * 11,
        out_specs=VM,
        compiler_params=pltpu.CompilerParams(vmem_limit_bytes=24 * 1024 * 1024),
        cost_estimate=pl.CostEstimate(flops=2 * 192 * 1024 * 2048, bytes_accessed=6_000_000, transcendentals=0),
        name="down",
    )(z.reshape(1), c.reshape(1), mine, other, *weights)


def layer(
    tokens,
    state,
    w_query,
    w_key,
    w_value,
    w_gate,
    w_decay,
    w_beta,
    decay_rate,
    decay_bias,
    mix_gain,
    out_gain,
    w_out,
    ffn_gain,
    w_up,
    w_down,
):
    _, width = tokens.shape
    _, _, z, c = (lax.axis_index(axis).astype(jnp.int32) for axis in EVERYWHERE)
    tp = z * 2 + c
    half = w_up.shape[1] // 2
    everything = lax.all_gather(tokens, TP, axis=0, tiled=False)
    new_state, keep, give = attn(
        everything, (tp * 2).reshape(1), c.reshape(1), w_query, w_key, w_value, w_gate, w_decay, w_beta, w_out,
        decay_rate, decay_bias, mix_gain, out_gain, state,
    )
    took = other_core(give)
    parts = lax.all_to_all(pair_sum(keep, took), "z", 0, 0, tiled=True)
    w_up = tied(w_up, give)
    up_mine = lax.dynamic_slice_in_dim(w_up, c * half, half, 1)
    up_other = other_core(lax.dynamic_slice_in_dim(w_up, (1 - c) * half, half, 1))
    gain = lax.dynamic_slice_in_dim(ffn_gain, tp * width, width, 0).reshape(1, width)
    resid, send = residual(tokens, gain, parts)
    mine = lax.all_to_all(send, KV, 0, 0, tiled=True)
    theirs = other_core(mine)
    blocks = up_product(z, mine, theirs, up_mine, up_other)
    down_weights = ring_gather(w_down, everything, None, send, mine)
    hidden = finish_hidden(*ring_sum(blocks))
    down = down_product(z, c, hidden, other_core(hidden), down_weights)
    down = lax.all_to_all(down, KV, 0, 0, tiled=True)
    down = down.astype(F32).sum(axis=0).astype(BF16)
    routes = [
        (((2 * a + b) * 8 + s) * 2 + k, ((2 * s + b) * 8 + (a - s) % 8) * 2 + k)
        for a in range(8) for b in range(2) for s in range(8) for k in range(2)
    ]
    down = lax.ppermute(down, EVERYWHERE, routes)
    mixed = (resid + down.astype(F32)).astype(BF16)
    return (mixed, new_state)


def solution(mesh):
    split = Mesh(mesh.devices.reshape(4, 4, 8, 2), EVERYWHERE)
    placed = (
        P(KV, TP),
        P(KV, TP, None),
        P(None, TP),
        P(None, TP),
        P(None, TP),
        P(None, TP),
        P(),
        P(),
        P(TP),
        P(TP),
        P(),
        P(),
        P(TP, None),
        P(),
        P(TP, KV),
        P(KV, TP),
    )
    return jax.shard_map(
        layer,
        mesh=split,
        in_specs=placed,
        out_specs=(P(KV, TP), P(KV, TP, None)),
        check_vma=False,
    )
```

```python
import functools

import jax
import jax.numpy as jnp
from jax import lax
from jax.experimental import pallas as pl
from jax.experimental.pallas import tpu as pltpu
from jax.sharding import Mesh
from jax.sharding import PartitionSpec as P

D = 4096
EPS = 1e-06
F32 = jnp.float32
BF16 = jnp.bfloat16
TP = ("z", "c")
KV = ("y", "x")
EVERYWHERE = ("y", "x", "z", "c")
PAD = 8


def attn_kernel(h0_ref, core_ref, rate_ref, bias_ref, tok_ref, mg_ref, wq_hbm, wk_hbm, wv_hbm, wg_hbm, wd_hbm, wb_hbm, wo_hbm, og_ref, st_hbm,
                kept_ref, keep_ref, give_ref, wo, w4, w2, st, xn, vv, od, ex, e2, sem_w, sem_in):
    rows = tok_ref.shape[1]
    width = tok_ref.shape[2]
    parts = tok_ref.shape[0]
    nt = rows // 8
    loads = [pltpu.make_async_copy(src, w4.at[i], sem_w.at[i]) for i, src in enumerate((wq_hbm, wk_hbm, wv_hbm, wg_hbm))]
    loads += [pltpu.make_async_copy(src, w2.at[i], sem_w.at[4 + i]) for i, src in enumerate((wd_hbm, wb_hbm))]
    loads += [pltpu.make_async_copy(wo_hbm, wo, sem_w.at[6])]
    cin = pltpu.make_async_copy(st_hbm, st, sem_in)
    loads[1].start()
    loads[0].start()
    ei = lax.broadcasted_iota(jnp.int32, e2.shape, 0)
    ec = lax.broadcasted_iota(jnp.int32, e2.shape, 1)
    e2[...] = jnp.where((ei & 63) == (ec >> 6), 1.0, 0.0).astype(BF16)
    ss = jnp.zeros((rows, width), F32)
    for t in range(parts):
        x = tok_ref[t].astype(F32)
        ss = ss + x * x
    for i in (4, 5, 2):
        loads[i].start()
    cin.start()
    r = lax.rsqrt(jnp.sum(ss, axis=-1, keepdims=True) / (parts * width) + EPS)
    for t in range(parts):
        xn[:, t * width:(t + 1) * width] = (tok_ref[t].astype(F32) * r * mg_ref[t]).astype(BF16)
    x = xn[...]

    def proj(i):
        loads[i].wait()
        return jnp.dot(x, w4[i], preferred_element_type=F32)

    lane = lax.broadcasted_iota(jnp.int32, (rows, 128), 1)
    lo = lane < 64

    def halves(a):
        s0 = jnp.sum(jnp.where(lo, a, 0.0), axis=-1, keepdims=True)
        s1 = jnp.sum(jnp.where(lo, 0.0, a), axis=-1, keepdims=True)
        return s0, s1

    def spread(s):
        return jnp.where(lo, s[0], s[1])

    def expand(a, slot):
        hi = a.astype(BF16).astype(F32)
        low = a - hi
        for h in range(2):
            if h == 0:
                both = jnp.where(lo, hi, pltpu.roll(low, 64, 1))
            else:
                both = jnp.where(lo, pltpu.roll(hi, 64, 1), low)
            ex[slot + h] = jnp.dot(both.astype(BF16), e2[...], preferred_element_type=F32)

    k = proj(1)
    ks = k * lax.rsqrt(spread(halves(k * k)) + EPS)
    expand(ks, 0)
    kept_ref[0] = ks
    loads[3].start()
    loads[6].start()
    q = proj(0)
    qs = q * lax.rsqrt(spread(halves(q * q)) + EPS) * (64 ** -0.5)
    expand(qs, 2)
    nt_dims = (((1,), (1,)), ((), ()))
    loads[4].wait()
    loads[5].wait()
    pd = lax.dot_general(x, w2[0], nt_dims, preferred_element_type=F32)
    pb = lax.dot_general(x, w2[1], nt_dims, preferred_element_type=F32)
    v = proj(2)
    vr = pltpu.roll(v, 64, 1)
    vv[0] = jnp.where(lo, v, vr)
    vv[1] = jnp.where(lo, vr, v)
    kq = halves(qs * ks)
    hl = lax.broadcasted_iota(jnp.int32, pd.shape, 1)
    h0 = h0_ref[0]
    for h in range(2):
        sel = hl == h0 + h
        d = jnp.sum(jnp.where(sel, pd, 0.0), axis=-1, keepdims=True) + bias_ref[h]
        sp = jnp.maximum(d, 0.0) + jnp.log1p(jnp.exp(-jnp.abs(d)))
        dec = jnp.exp(-rate_ref[h] * sp)
        b = jnp.sum(jnp.where(sel, pb, 0.0), axis=-1, keepdims=True)
        stren = 1.0 / (1.0 + jnp.exp(-b))
        od[h, 0] = jnp.broadcast_to(dec, (rows, 128))
        kept_ref[3 + h] = jnp.broadcast_to(dec, (rows, 128))
        od[h, 1] = jnp.broadcast_to(stren, (rows, 128))
        od[h, 2] = jnp.broadcast_to(kq[h], (rows, 128))
    cin.wait()

    def body(bt, _):
        r0 = pl.multiple_of(bt * 8, 8)
        for h in range(2):
            rec = jnp.zeros((8, 128), F32)
            out = jnp.zeros((8, 128), F32)
            for j in range(32):
                s = st[pl.ds(bt * 512 + 2 * j + h, 8, stride=64), :]
                ke = ex[h, pl.ds(r0, 8), j * 128:(j + 1) * 128]
                qe = ex[2 + h, pl.ds(r0, 8), j * 128:(j + 1) * 128]
                rec = rec + s * ke
                out = out + s * qe
            rec = rec + pltpu.roll(rec, 64, 1)
            out = out + pltpu.roll(out, 64, 1)
            dec = od[h, 0, pl.ds(r0, 8), :]
            stren = od[h, 1, pl.ds(r0, 8), :]
            kq8 = od[h, 2, pl.ds(r0, 8), :]
            delta = stren * (vv[h, pl.ds(r0, 8), :] - dec * rec)
            od[h, 3, pl.ds(r0, 8), :] = dec * out + kq8 * delta
            kept_ref[1 + h, pl.ds(r0, 8), :] = delta
        return 0

    lax.fori_loop(0, nt, body, 0)
    g = proj(3)
    o = jnp.where(lo, od[0, 3], od[1, 3])
    ms = spread(halves(o * o)) * (1.0 / 64)
    gain = jnp.concatenate([og_ref[...], og_ref[...]], axis=1)
    ho = o * lax.rsqrt(ms + EPS) * gain * (g / (1.0 + jnp.exp(-g)))
    head_out = ho.astype(BF16)
    loads[6].wait()
    core = core_ref[0]
    for i in range(keep_ref.shape[0]):
        for ref, side in ((give_ref, 1 - core), (keep_ref, core)):
            cols = wo[:, pl.ds(pl.multiple_of((2 * i + side) * width, width), width)]
            ref[i] = jnp.dot(head_out, cols, preferred_element_type=F32).astype(BF16)


def attn(tok, h0, core, wq, wk, wv, wg, wd, wb, wo, rate, bias, mix_gain, out_gain, state):
    parts, rows, width = tok.shape
    mg = mix_gain.reshape(parts, 1, width)
    heads = state.shape[1]
    st = state.reshape(rows, heads, 32, 128).transpose(0, 2, 1, 3).reshape(rows * 64, 128)
    vm = pl.BlockSpec(memory_space=pltpu.VMEM)
    sm = pl.BlockSpec(memory_space=pltpu.SMEM)
    an = pl.BlockSpec(memory_space=pl.ANY)
    kept, keep, give = pl.pallas_call(
        attn_kernel,
        out_shape=(jax.ShapeDtypeStruct((5, rows, 128), F32), jax.ShapeDtypeStruct((8, rows, width), BF16), jax.ShapeDtypeStruct((8, rows, width), BF16)),
        in_specs=[sm, sm, sm, sm, vm, vm] + [an] * 7 + [vm, an],
        out_specs=(vm, vm, vm),
        scratch_shapes=[
            pltpu.VMEM(wo.shape, BF16),
            pltpu.VMEM((4,) + wq.shape, BF16),
            pltpu.VMEM((2,) + wd.shape[::-1], BF16),
            pltpu.VMEM((rows * 64, 128), F32),
            pltpu.VMEM((rows, parts * width), BF16),
            pltpu.VMEM((2, rows, 128), F32),
            pltpu.VMEM((2, 4, rows, 128), F32),
            pltpu.VMEM((4, rows, 4096), F32),
            pltpu.VMEM((128, 4096), BF16),
            pltpu.SemaphoreType.DMA((7,)),
            pltpu.SemaphoreType.DMA,
        ],
        compiler_params=pltpu.CompilerParams(vmem_limit_bytes=56 * 1024 * 1024),
        cost_estimate=pl.CostEstimate(flops=2 * 96 * 4096 * 600, bytes_accessed=12_000_000, transcendentals=50000),
        name="attn",
    )(h0, core, rate, bias, tok, mg, wq, wk, wv, wg, wd.T, wb.T, wo, out_gain.reshape(1, 64), st)
    return kept, keep, give


def state_kernel(kept_ref, st_ref, *refs):
    out_ref = refs[-1]
    lane = lax.broadcasted_iota(jnp.int32, (8, 128), 1)
    upper = lane >> 6
    for h in range(2):
        key = kept_ref[0]
        delta = kept_ref[1 + h]
        decay = kept_ref[3 + h]
        for j in range(32):
            at = pl.ds(2 * j + h, 8, stride=64)
            spread = jnp.take_along_axis(key, upper + (64 * h + 2 * j), axis=1)
            out_ref[at, :] = decay * st_ref[at, :] + spread * delta


def next_state(kept, state, base, steps, partial=None):
    rows, heads, _ = state.shape
    st = state.reshape(rows, heads, 32, 128).transpose(0, 2, 1, 3).reshape(rows * 64, 128)
    block = pl.BlockSpec((512, 128), lambda i: (i + base, 0))
    operands = (kept, st) if partial is None else (kept, st, partial)
    return pl.pallas_call(
        state_kernel,
        grid=(steps,),
        out_shape=jax.ShapeDtypeStruct((rows * 64, 128), F32),
        in_specs=[pl.BlockSpec((5, 8, 128), lambda i: (0, i + base, 0)), block]
        + [pl.BlockSpec(memory_space=pl.ANY)] * (len(operands) - 2),
        out_specs=block,
        input_output_aliases={} if partial is None else {2: 0},
        compiler_params=pltpu.CompilerParams(vmem_limit_bytes=56 * 1024 * 1024),
        cost_estimate=pl.CostEstimate(flops=10_000_000, bytes_accessed=3_200_000, transcendentals=0),
        name="next",
    )(*operands)


VM = pl.BlockSpec(memory_space=pltpu.VMEM)
SM = pl.BlockSpec(memory_space=pltpu.SMEM)


def shifted(array, by, axis="z"):
    length = lax.axis_size(axis)
    return lax.ppermute(array, axis, [(i, (i + by) % length) for i in range(length)])


def other_core(array):
    return lax.ppermute(array, "c", [(0, 1), (1, 0)])


def out_kernel(tp_ref, tok_ref, gain_ref, parts_ref, resid_ref, send_ref):
    rows, width = tok_ref.shape
    acc = tok_ref[...].astype(F32)
    for i in range(parts_ref.shape[0]):
        acc = acc + parts_ref[i].astype(F32)
    resid_ref[...] = acc
    squares = jnp.sum(acc * acc, axis=-1, keepdims=True)
    eye = lax.broadcasted_iota(jnp.int32, (rows, 128), 0) == lax.broadcasted_iota(jnp.int32, (rows, 128), 1)
    flat = jnp.sum(jnp.where(eye, squares, 0.0), axis=0, keepdims=True)
    scaled = (acc * gain_ref[tp_ref[0]]).astype(BF16)
    extra = jnp.broadcast_to(flat, (PAD, 128)).astype(BF16)
    blank = jnp.zeros((PAD, width - 128), BF16)
    for i in range(send_ref.shape[0]):
        send_ref[i, :rows, :] = scaled
        send_ref[i, rows:, :128] = extra
        send_ref[i, rows:, 128:] = blank


def residual(tp, tokens, gain, parts):
    rows, width = tokens.shape
    return pl.pallas_call(
        out_kernel,
        out_shape=(jax.ShapeDtypeStruct((rows, width), F32), jax.ShapeDtypeStruct((16, rows + PAD, width), BF16)),
        in_specs=[SM] + [VM] * 3,
        out_specs=(VM, VM),
        compiler_params=pltpu.CompilerParams(vmem_limit_bytes=16 * 1024 * 1024),
        cost_estimate=pl.CostEstimate(flops=1_000_000, bytes_accessed=2_000_000, transcendentals=0),
        name="out",
    )(tp.reshape(1), tokens, gain, parts)


def up_kernel(z_ref, c_ref, mine_ref, other_ref, wu_ref, wo_ref, *outs):
    rows = mine_ref.shape[1] - PAD
    width = mine_ref.shape[2]
    wide = wo_ref.shape[1]
    w_mine = wu_ref[:, pl.ds(pl.multiple_of(c_ref[0] * wide, wide), wide)]
    for o in (4, 3, 5, 2, 6, 1, 7, 0):
        at = (z_ref[0] + o) & 7
        own = mine_ref[pl.ds(2 * at, 2)]
        his = other_ref[pl.ds(2 * at, 2)]
        product = (
            jnp.dot(own[:, :rows].reshape(2 * rows, width), w_mine, preferred_element_type=F32)
            + jnp.dot(his[:, :rows].reshape(2 * rows, width), wo_ref[...], preferred_element_type=F32)
        ).astype(BF16)
        squares = own[:, rows:, :128].astype(F32) + his[:, rows:, :128].astype(F32)
        side = product.shape[1] // 2
        left, right = outs[o], outs[o]
        shift = side
        if o == 4:
            right, shift = outs[8], 0
        left[: 2 * rows, :side] = product[:, :side]
        left[2 * rows :, :128] = squares[0].astype(BF16)
        left[2 * rows :, 128:256] = squares[1].astype(BF16)
        right[: 2 * rows, shift : shift + side] = product[:, side:]
        right[2 * rows :, shift : shift + side] = jnp.zeros((PAD, side), BF16)


def up_product(z, c, mine, other, w_up, w_other):
    rows = mine.shape[1] - PAD
    return pl.pallas_call(
        up_kernel,
        out_shape=tuple(
            jax.ShapeDtypeStruct((2 * rows + PAD, w_other.shape[1] // (2 if o in (4, 8) else 1)), BF16) for o in range(9)
        ),
        in_specs=[SM, SM] + [VM] * 4,
        out_specs=tuple([VM] * 9),
        compiler_params=pltpu.CompilerParams(vmem_limit_bytes=24 * 1024 * 1024),
        cost_estimate=pl.CostEstimate(flops=2 * 1536 * 512 * 512, bytes_accessed=4_000_000, transcendentals=0),
        name="up",
    )(z.reshape(1), c.reshape(1), mine, other, w_up, w_other)


def hidden_kernel(a_ref, b_ref, c_ref, out_ref):
    total = a_ref[...].astype(F32) + b_ref[...].astype(F32) + c_ref[...].astype(F32)
    both = out_ref.shape[0]
    rows = both // 2
    eye = lax.broadcasted_iota(jnp.int32, (rows, 128), 0) == lax.broadcasted_iota(jnp.int32, (rows, 128), 1)
    for b in range(2):
        flat = total[both : both + 1, b * 128 : (b + 1) * 128]
        squares = jnp.sum(jnp.where(eye, flat, 0.0), axis=1, keepdims=True)
        up = jnp.maximum(total[b * rows : (b + 1) * rows], 0.0)
        out_ref[b * rows : (b + 1) * rows, :] = (up * up / (squares / D + EPS)).astype(BF16)


def finish_hidden(first, second, third):
    return pl.pallas_call(
        hidden_kernel,
        out_shape=jax.ShapeDtypeStruct((first.shape[0] - PAD, first.shape[1]), BF16),
        in_specs=[VM] * 3,
        out_specs=VM,
        compiler_params=pltpu.CompilerParams(vmem_limit_bytes=16 * 1024 * 1024),
        cost_estimate=pl.CostEstimate(flops=1_000_000, bytes_accessed=800_000, transcendentals=0),
        name="hidden",
    )(first, second, third)


def pair_kernel(one_ref, two_ref, out_ref):
    out_ref[...] = (one_ref[...].astype(F32) + two_ref[...].astype(F32)).astype(BF16)


def pair_sum(one, two):
    return pl.pallas_call(
        pair_kernel,
        out_shape=jax.ShapeDtypeStruct(one.shape, BF16),
        in_specs=[VM] * 2,
        out_specs=VM,
        compiler_params=pltpu.CompilerParams(vmem_limit_bytes=16 * 1024 * 1024),
        cost_estimate=pl.CostEstimate(flops=1_000_000, bytes_accessed=1_000_000, transcendentals=0),
        name="pair",
    )(one, two)


def total_kernel(parts_ref, out_ref):
    total = parts_ref[0].astype(F32)
    for i in range(1, parts_ref.shape[0]):
        total = total + parts_ref[i].astype(F32)
    out_ref[...] = total.astype(BF16)


def total_of(parts):
    return pl.pallas_call(
        total_kernel,
        out_shape=jax.ShapeDtypeStruct(parts.shape[1:], BF16),
        in_specs=[VM],
        out_specs=VM,
        compiler_params=pltpu.CompilerParams(vmem_limit_bytes=4 * 1024 * 1024),
        cost_estimate=pl.CostEstimate(flops=500_000, bytes_accessed=900_000, transcendentals=0),
        name="total",
    )(parts)


def other_half_kernel(c_ref, w_ref, out_ref):
    half = out_ref.shape[1]
    out_ref[...] = w_ref[:, pl.ds(pl.multiple_of((1 - c_ref[0]) * half, half), half)]


def other_half(c, w):
    return pl.pallas_call(
        other_half_kernel,
        out_shape=jax.ShapeDtypeStruct((w.shape[0], w.shape[1] // 2), BF16),
        in_specs=[SM, VM],
        out_specs=VM,
        compiler_params=pltpu.CompilerParams(vmem_limit_bytes=4 * 1024 * 1024),
        cost_estimate=pl.CostEstimate(flops=100_000, bytes_accessed=800_000, transcendentals=0),
        name="other",
    )(c.reshape(1), w)


def half_kernel(start, full_ref, part_ref, out_ref):
    out_ref[...] = full_ref[...]
    cols = slice(start, start + part_ref.shape[1])
    out_ref[:, cols] = (full_ref[:, cols].astype(F32) + part_ref[...].astype(F32)).astype(BF16)


def half_sum(full, part, start):
    return pl.pallas_call(
        functools.partial(half_kernel, start),
        out_shape=jax.ShapeDtypeStruct(full.shape, BF16),
        in_specs=[VM] * 2,
        out_specs=VM,
        compiler_params=pltpu.CompilerParams(vmem_limit_bytes=8 * 1024 * 1024),
        cost_estimate=pl.CostEstimate(flops=100_000, bytes_accessed=500_000, transcendentals=0),
        name="half",
    )(full, part)


def ring_sum(blocks):
    ahead = shifted(blocks[4], 1)
    back = shifted(blocks[8], -1)
    ahead = half_sum(blocks[3], ahead, 0)
    ahead = shifted(ahead, 1)
    back = half_sum(blocks[5], back, blocks[4].shape[1])
    back = shifted(back, -1)
    for step in (2, 1):
        ahead = pair_sum(blocks[step], ahead)
        ahead = shifted(ahead, 1)
        back = pair_sum(blocks[8 - step], back)
        back = shifted(back, -1)
    return blocks[0], ahead, back


def tied(array, *others):
    return lax.optimization_barrier((array,) + others)[0]


def ring_gather(block, *after):
    parts = [None] * 8
    parts[0] = block
    half = block.shape[0] // 2
    ahead = behind = block
    for step in range(1, 4):
        if after[step - 1] is not None:
            ahead, behind, _ = lax.optimization_barrier((ahead, behind, after[step - 1]))
        behind = shifted(behind, 1)
        ahead = shifted(ahead, -1)
        parts[8 - step] = behind
        parts[step] = ahead
    ahead, behind, _ = lax.optimization_barrier((ahead, behind, after[3]))
    low = shifted(ahead[:half], -1)
    high = shifted(behind[half:], 1)
    parts[4:5] = [low, high]
    return parts


def down_kernel(z_ref, c_ref, mine_ref, other_ref, *refs):
    weights, out_ref = refs[:-1], refs[-1]
    rows = out_ref.shape[1]
    half = mine_ref.shape[1]
    flip = jnp.broadcast_to(c_ref[0], mine_ref.shape) > 0
    mine = mine_ref[...].astype(F32)
    other = other_ref[...].astype(F32)
    low = jnp.where(flip, other, mine).astype(BF16)
    high = jnp.where(flip, mine, other).astype(BF16)
    for o in range(8):
        if o == 4:
            top, bottom = weights[4][...], weights[5][...]
        else:
            ref = weights[o] if o < 4 else weights[o + 1]
            top, bottom = ref[:half, :], ref[half:, :]
        out = jnp.dot(low, top, preferred_element_type=F32) + jnp.dot(high, bottom, preferred_element_type=F32)
        at = (o + 2 * z_ref[0]) & 7
        out_ref[2 * at] = out[:rows].astype(BF16)
        out_ref[2 * at + 1] = out[rows:].astype(BF16)


def down_product(z, c, mine, other, weights):
    rows = mine.shape[0] // 2
    width = weights[0].shape[1]
    return pl.pallas_call(
        down_kernel,
        out_shape=jax.ShapeDtypeStruct((16, rows, width), BF16),
        in_specs=[SM, SM] + [VM] * 11,
        out_specs=VM,
        compiler_params=pltpu.CompilerParams(vmem_limit_bytes=24 * 1024 * 1024),
        cost_estimate=pl.CostEstimate(flops=2 * 192 * 1024 * 2048, bytes_accessed=6_000_000, transcendentals=0),
        name="down",
    )(z.reshape(1), c.reshape(1), mine, other, *weights)


def layer(
    tokens,
    state,
    w_query,
    w_key,
    w_value,
    w_gate,
    w_decay,
    w_beta,
    decay_rate,
    decay_bias,
    mix_gain,
    out_gain,
    w_out,
    ffn_gain,
    w_up,
    w_down,
):
    rows, width = tokens.shape
    _, _, z, c = (lax.axis_index(axis).astype(jnp.int32) for axis in EVERYWHERE)
    tp = z * 2 + c
    everything = lax.all_gather(tokens, TP, axis=0, tiled=False)
    kept, keep, give = attn(
        everything, (tp * 2).reshape(1), c.reshape(1), w_query, w_key, w_value, w_gate, w_decay, w_beta, w_out,
        decay_rate, decay_bias, mix_gain, out_gain, state,
    )
    took = other_core(give)
    parts = lax.all_to_all(pair_sum(keep, took), "z", 0, 0, tiled=True)
    w_up = tied(w_up, give)
    up_send = other_half(c, w_up)
    up_other = other_core(up_send)
    half_state = next_state(kept, state, 0, 6)
    resid, send = residual(tp, tokens, ffn_gain.reshape(16, 1, width), parts)
    mine = lax.all_to_all(send, KV, 0, 0, tiled=True)
    theirs = other_core(mine)
    blocks = up_product(z, c, mine, theirs, w_up, up_other)
    down_weights = ring_gather(w_down, everything, None, send, mine)
    hidden = finish_hidden(*ring_sum(blocks))
    down = down_product(z, c, hidden, other_core(hidden), down_weights)
    half_state = next_state(kept, state, 6, 3, half_state)
    new_state = next_state(kept, state, 9, 3, half_state)
    new_state = new_state.reshape(rows, 32, 2, 128).transpose(0, 2, 1, 3).reshape(state.shape)
    down = lax.all_to_all(down, KV, 0, 0, tiled=True)
    down = total_of(down)
    routes = [
        (((2 * a + b) * 8 + s) * 2 + k, ((2 * s + b) * 8 + (a - s) % 8) * 2 + k)
        for a in range(8) for b in range(2) for s in range(8) for k in range(2)
    ]
    down = lax.ppermute(down, EVERYWHERE, routes)
    mixed = (resid + down.astype(F32)).astype(BF16)
    return (mixed, new_state)


def solution(mesh):
    split = Mesh(mesh.devices.reshape(4, 4, 8, 2), EVERYWHERE)
    placed = (
        P(KV, TP),
        P(KV, TP, None),
        P(None, TP),
        P(None, TP),
        P(None, TP),
        P(None, TP),
        P(),
        P(),
        P(TP),
        P(TP),
        P(),
        P(),
        P(TP, None),
        P(),
        P(TP, KV),
        P(KV, TP),
    )
    return jax.shard_map(
        layer,
        mesh=split,
        in_specs=placed,
        out_specs=(P(KV, TP), P(KV, TP, None)),
        check_vma=False,
    )
```
